32 devices in a mesh: fs: 8 (over z, y), tp: 4 (over x, core).
Axes of the slice: x: 2, y: 2, z: 4, core: 2. Of those that a mesh axis runs over, the one named last changes fastest.
Arguments:
- tokens: bfloat16 [8192, 2048], P(('fs', 'tp')), may hold values from -6 to 6
- first_block_norm_scale: float32 [2048], replicated, may hold values from 0.1 to 1.9
- first_block_gate_matrix: bfloat16 [2048, 5504], P('fs', 'tp'), may hold values from -0.125 to 0.125
- first_block_up_matrix: bfloat16 [2048, 5504], P('fs', 'tp'), may hold values from -0.125 to 0.125
- first_block_down_matrix: bfloat16 [5504, 2048], P('tp', 'fs'), may hold values from -0.078125 to 0.078125
- mixer_norm_scale: float32 [2048], replicated, may hold values from 0.1 to 1.9
- recurrent_input_matrix: bfloat16 [2048, 3072], P('fs', 'tp'), may hold values from -0.125 to 0.125
- output_gate_projection: bfloat16 [2048, 3072], P('fs', 'tp'), may hold values from -0.125 to 0.125
- convolution_kernel: float32 [4, 3072], P(None, 'tp'), may hold values from -2 to 2
- decay_gate_blocks: bfloat16 [16, 192, 192], P('tp'), may hold values from -0.4375 to 0.4375
- input_gate_blocks: bfloat16 [16, 192, 192], P('tp'), may hold values from -0.4375 to 0.4375
- channel_decay_weight: float32 [3072], P('tp'), may hold values from 3.5 to 11.5
- position_decay_extra: float32 [8192], P('fs'), may hold values from -0.7 to 0
- mixer_output_matrix: bfloat16 [3072, 2048], P('tp', 'fs'), may hold values from -0.109375 to 0.109375
- second_block_norm_scale: float32 [2048], replicated, may hold values from 0.1 to 1.9
- second_block_gate_matrix: bfloat16 [2048, 5504], P('fs', 'tp'), may hold values from -0.125 to 0.125
- second_block_up_matrix: bfloat16 [2048, 5504], P('fs', 'tp'), may hold values from -0.125 to 0.125
- second_block_down_matrix: bfloat16 [5504, 2048], P('tp', 'fs'), may hold values from -0.078125 to 0.078125
Outputs:
- layer_out: bfloat16 [8192, 2048], P(('fs', 'tp'))
The draws below stay inside these ranges and needn't reach their ends.
All inputs are finite; a program needn't handle non-finite values.
Results may differ from the reference program's by a relative error of at most 0.019.
Values may be sent and summed in bfloat16 or wider, within the bound.
A program may use at most 128 MiB of HBM per device.

```python
import jax
import jax.numpy as jnp
from jax import lax

D = 2048
FF = 5504
DR = 3072
RB = 16
BLK = 192
CONV = 4
SEQUENCE_TOKENS = 1024
TOKENS = 8192
N_TP = 4


def draw_channel_decay_weight(key, part):
    pick_key = jax.random.fold_in(key, 11)
    slow_key = jax.random.fold_in(key, 12)
    quick_key = jax.random.fold_in(key, 13)
    fraction = 0.5
    quick_mask = jax.random.bernoulli(pick_key, fraction, (DR,))
    slow_log = jax.random.uniform(slow_key, (DR,), jnp.float32, minval=jnp.log(2e-05), maxval=jnp.log(0.00025))
    quick_log = jax.random.uniform(quick_key, (DR,), jnp.float32, minval=jnp.log(0.004), maxval=jnp.log(0.02))
    softened = jnp.exp(jnp.where(quick_mask, quick_log, slow_log))
    return (-jnp.log(jnp.expm1(softened))).astype(jnp.float32)


def draw_position_decay_extra(key, part):
    where_key = jax.random.fold_in(key, 21)
    depth_key = jax.random.fold_in(key, 22)
    struck = jax.random.bernoulli(where_key, 4.0 / SEQUENCE_TOKENS, (TOKENS,))
    strength = jax.random.uniform(depth_key, (TOKENS,), jnp.float32, minval=jnp.log(0.5), maxval=jnp.log(0.8))
    return jnp.where(struck, strength, 0.0).astype(jnp.float32)


def block_scale(rng, dims, cuts, least, largest):
    def one(dim, parts):
        draws = jax.random.uniform(jax.random.fold_in(jax.random.fold_in(rng, 6), dim), (parts,), jnp.float32, least / len(cuts), largest / len(cuts))
        return jnp.repeat(jnp.exp(draws), dims[dim] // parts).reshape((-1,) + (1,) * (len(dims) - dim - 1))

    level = one(*cuts[0])
    for cut in cuts[1:]:
        level = level * one(*cut)
    return level


def centred(own_key, dims, spread, reach, cuts=(), dtype=jnp.bfloat16):
    loudness = block_scale(own_key, dims, cuts, -0.22, 0.18) if cuts else 1.0
    values = jax.random.normal(own_key, dims, jnp.float32) * spread * loudness
    return jnp.minimum(jnp.maximum(values, -reach), reach).astype(dtype)


def setup_inputs(seed: int = 0) -> dict:
    arg_keys = jax.random.split(jax.random.key(seed), 19)
    return {
        "tokens": centred(arg_keys[0], (TOKENS, D), 1.0, 6.0, ((0, 32),)),
        "first_block_norm_scale": jnp.clip(1.0 + 0.18 * jax.random.normal(arg_keys[1], (D,), jnp.float32), 0.1, 1.9),
        "first_block_gate_matrix": centred(arg_keys[2], (D, FF), D ** -0.5, 0.125, ((0, 8), (1, 4))),
        "first_block_up_matrix": centred(arg_keys[3], (D, FF), D ** -0.5, 0.125, ((0, 8), (1, 4))),
        "first_block_down_matrix": centred(arg_keys[4], (FF, D), FF ** -0.5, 0.078125, ((0, 4), (1, 8))),
        "mixer_norm_scale": jnp.clip(1.0 + 0.18 * jax.random.normal(arg_keys[5], (D,), jnp.float32), 0.1, 1.9),
        "recurrent_input_matrix": centred(arg_keys[6], (D, DR), D ** -0.5, 0.125, ((0, 8), (1, 4))),
        "output_gate_projection": centred(arg_keys[7], (D, DR), D ** -0.5, 0.125, ((0, 8), (1, 4))),
        "convolution_kernel": centred(arg_keys[8], (CONV, DR), 0.5, 2.0, ((1, 4),), jnp.float32),
        "decay_gate_blocks": centred(arg_keys[9], (RB, BLK, BLK), BLK ** -0.5, 0.4375, ((0, 4),)),
        "input_gate_blocks": centred(arg_keys[10], (RB, BLK, BLK), BLK ** -0.5, 0.4375, ((0, 4),)),
        "channel_decay_weight": draw_channel_decay_weight(jax.random.fold_in(arg_keys[18], 71), 0),
        "position_decay_extra": draw_position_decay_extra(jax.random.fold_in(arg_keys[18], 71), 0),
        "mixer_output_matrix": centred(arg_keys[13], (DR, D), DR ** -0.5, 0.109375, ((0, 4), (1, 8))),
        "second_block_norm_scale": jnp.clip(1.0 + 0.18 * jax.random.normal(arg_keys[14], (D,), jnp.float32), 0.1, 1.9),
        "second_block_gate_matrix": centred(arg_keys[15], (D, FF), D ** -0.5, 0.125, ((0, 8), (1, 4))),
        "second_block_up_matrix": centred(arg_keys[16], (D, FF), D ** -0.5, 0.125, ((0, 8), (1, 4))),
        "second_block_down_matrix": centred(arg_keys[17], (FF, D), FF ** -0.5, 0.078125, ((0, 4), (1, 8))),
    }


EPS = 1e-06
RECURRENT_WIDTH = 8.0

def normed(input_token_rows, norm_scale_vector):
    values = input_token_rows.astype(jnp.float32)
    square = lax.optimization_barrier(jnp.mean(values * values, axis=-1, keepdims=True))
    return (values * lax.rsqrt(square + EPS) * norm_scale_vector).astype(jnp.bfloat16)

def block_sum(hidden, weight):
    span_width = hidden.shape[1] // N_TP
    running = jnp.zeros((hidden.shape[0], weight.shape[1]), jnp.float32)
    for index_k in range(N_TP):
        lower = index_k * span_width
        partial_sum = jnp.dot(hidden[:, lower:lower + span_width], weight[lower:lower + span_width], preferred_element_type=jnp.float32).astype(jnp.bfloat16)
        partial_sum = lax.optimization_barrier(partial_sum)
        running = running + partial_sum.astype(jnp.float32)
    return running

def feed_forward(input_token_rows, norm_scale_vector, gate_weight, up_weight, down_weight):
    normal = normed(input_token_rows, norm_scale_vector)
    gate_pre = jnp.dot(normal, gate_weight, preferred_element_type=jnp.float32)
    up_pre = jnp.dot(normal, up_weight, preferred_element_type=jnp.float32)
    hidden = (jax.nn.silu(gate_pre) * up_pre).astype(jnp.bfloat16)
    return block_sum(hidden, down_weight)

def blockwise(values, weight):
    dims_in = values.shape
    grouped = values.reshape(dims_in[:-1] + (weight.shape[0], weight.shape[1])).astype(jnp.float32)
    result = jnp.einsum('sthi,hij->sthj', grouped, weight.astype(jnp.float32))
    return result.reshape(dims_in)

def combine(earlier, later):
    decay_one, drive_one = earlier
    decay_two, drive_two = later
    return (decay_one * decay_two, decay_two * drive_one + drive_two)

def linear_recurrence_scan(input_token_rows, norm_scale_vector, recurrent_input_matrix, output_gate_projection, convolution_kernel, decay_gate_blocks, input_gate_blocks, channel_decay_weight, position_decay_extra, mixer_output_matrix):
    normal = normed(input_token_rows, norm_scale_vector)
    sequence_batch_count = normal.shape[0] // SEQUENCE_TOKENS
    recur_rows = jnp.dot(normal, recurrent_input_matrix, preferred_element_type=jnp.float32).astype(jnp.bfloat16)
    branch_rows = jnp.dot(normal, output_gate_projection, preferred_element_type=jnp.float32).astype(jnp.bfloat16)
    recur_rows = recur_rows.reshape(sequence_batch_count, SEQUENCE_TOKENS, -1)
    branch_rows = branch_rows.reshape(sequence_batch_count, SEQUENCE_TOKENS, -1)
    taps = convolution_kernel.shape[0]
    padded = jnp.pad(recur_rows, ((0, 0), (taps - 1, 0), (0, 0)))
    summed = jnp.zeros(recur_rows.shape, jnp.float32)
    for offset in range(taps):
        summed = summed + padded[:, offset:offset + SEQUENCE_TOKENS].astype(jnp.float32) * convolution_kernel[offset]
    conv_out = summed.astype(jnp.bfloat16)
    decay_gate_value = jax.nn.sigmoid(blockwise(conv_out, decay_gate_blocks))
    input_gate = jax.nn.sigmoid(blockwise(conv_out, input_gate_blocks))
    log_decay_factor = -RECURRENT_WIDTH * decay_gate_value * jax.nn.softplus(-channel_decay_weight) + position_decay_extra.reshape(sequence_batch_count, SEQUENCE_TOKENS, 1)
    decay_rate = jnp.exp(log_decay_factor)
    drive_in = jnp.sqrt(-jnp.expm1(2.0 * log_decay_factor)) * input_gate * conv_out.astype(jnp.float32)
    _, hidden_state = lax.associative_scan(combine, (decay_rate, drive_in), axis=1)
    gated = (jax.nn.gelu(branch_rows.astype(jnp.float32), approximate=True) * hidden_state).astype(jnp.bfloat16)
    return block_sum(gated.reshape(sequence_batch_count * SEQUENCE_TOKENS, -1), mixer_output_matrix)

def reference(tokens, first_block_norm_scale, first_block_gate_matrix, first_block_up_matrix, first_block_down_matrix, mixer_norm_scale, recurrent_input_matrix, output_gate_projection, convolution_kernel, decay_gate_blocks, input_gate_blocks, channel_decay_weight, position_decay_extra, mixer_output_matrix, second_block_norm_scale, second_block_gate_matrix, second_block_up_matrix, second_block_down_matrix):
    first_out = feed_forward(tokens, first_block_norm_scale, first_block_gate_matrix, first_block_up_matrix, first_block_down_matrix)
    residual_activations = (tokens.astype(jnp.float32) + 0.5 * first_out).astype(jnp.bfloat16)
    mixer_output_rows = linear_recurrence_scan(residual_activations, mixer_norm_scale, recurrent_input_matrix, output_gate_projection, convolution_kernel, decay_gate_blocks, input_gate_blocks, channel_decay_weight, position_decay_extra, mixer_output_matrix)
    residual_activations = (residual_activations.astype(jnp.float32) + mixer_output_rows).astype(jnp.bfloat16)
    second_out = feed_forward(residual_activations, second_block_norm_scale, second_block_gate_matrix, second_block_up_matrix, second_block_down_matrix)
    return (residual_activations.astype(jnp.float32) + 0.5 * second_out).astype(jnp.bfloat16)
```

```python
import functools

import jax
import jax.numpy as jnp
from jax import lax
from jax.experimental import pallas as pl
from jax.sharding import PartitionSpec as P


EPS = 1e-06
RECURRENT_WIDTH = 8.0
ROW_TILE = 128


def normed(input_token_rows, norm_scale_vector):
    values = input_token_rows.astype(jnp.float32)
    square = jnp.mean(values * values, axis=-1, keepdims=True)
    return (values * lax.rsqrt(square + EPS) * norm_scale_vector).astype(jnp.bfloat16)


def swap(value, axis, distance):
    size = lax.axis_size(axis)
    return lax.ppermute(value, axis, [(i, i ^ distance) for i in range(size)])


def order_pair(own, other, bit):
    return jnp.where(bit, other, own), jnp.where(bit, own, other)


def gather_rows(rows):
    size = lax.axis_size("tp")
    index = lax.axis_index("tp")
    held = rows[None]
    distance = size // 2
    while distance:
        other = swap(held, "tp", distance)
        low, high = order_pair(held, other, (index // distance) % 2 == 1)
        held = jnp.stack([low, high], axis=1).reshape((2 * held.shape[0],) + rows.shape)
        distance //= 2
    return held.reshape((-1,) + rows.shape[1:])


def half_of(rows, distance, bit):
    cut = rows.reshape((rows.shape[0] // (2 * distance), 2, distance) + rows.shape[1:])
    picked = lax.dynamic_index_in_dim(cut, bit, 1, keepdims=False)
    return picked.reshape((-1,) + rows.shape[1:])


def project_scatter(hidden, weight, row_count):
    size = lax.axis_size("tp")
    index = lax.axis_index("tp")
    blocks = hidden.reshape(size, row_count, hidden.shape[1])

    def product(part):
        flat = part.reshape(-1, part.shape[-1])
        out = jnp.dot(flat, weight, preferred_element_type=jnp.float32).astype(jnp.bfloat16)
        return out.reshape(part.shape[0], row_count, -1)

    bit = index % 2
    sent = swap(product(half_of(blocks, 1, 1 - bit)), "tp", 1)
    kept = product(half_of(blocks, 1, bit)).astype(jnp.float32) + sent.astype(jnp.float32)
    distance = 2
    while distance < size:
        bit = (index // distance) % 2
        cut = kept.reshape((-1, 2) + kept.shape[1:])
        mine = lax.dynamic_index_in_dim(cut, bit, 1, keepdims=False)
        theirs = lax.dynamic_index_in_dim(cut, 1 - bit, 1, keepdims=False)
        arrived = swap(theirs.astype(jnp.bfloat16), "tp", distance)
        kept = mine + arrived.astype(jnp.float32)
        distance *= 2
    return kept.reshape(row_count, -1)


def parity_groups(size):
    return [list(range(0, size, 2)), list(range(1, size, 2))]


def gather_weight(weight, dim):
    own = lax.all_gather(
        weight, "fs", axis=dim, tiled=True, axis_index_groups=parity_groups(lax.axis_size("fs"))
    )
    return own, swap(own, "fs", 1)


def split_features(rows):
    size = lax.axis_size("fs")
    bit = lax.axis_index("fs") % 2
    cut = rows.reshape(rows.shape[0], size // 2, 2, rows.shape[1] // size)
    even, odd = cut[:, :, 0].reshape(rows.shape[0], -1), cut[:, :, 1].reshape(rows.shape[0], -1)
    return order_pair(even, odd, bit == 1)


def join_features(own, other):
    size = lax.axis_size("fs")
    bit = lax.axis_index("fs") % 2
    even, odd = order_pair(own, other, bit == 1)
    shape = (own.shape[0], size // 2, own.shape[1] * 2 // size)
    return jnp.stack([even.reshape(shape), odd.reshape(shape)], axis=2).reshape(own.shape[0], -1)


def recurrence_kernel(
    recur_ref, branch_ref, taps_ref, decay_ref, input_ref, rate_ref, extra_ref, out_ref, *, tile
):
    length, width = recur_ref.shape
    taps = taps_ref.shape[0]

    def shifted(value, steps, fill):
        return jnp.concatenate(
            [jnp.full((steps, width), fill, jnp.float32), value[: tile - steps]], axis=0
        )

    def body(step, carry):
        tail, state = carry
        at = pl.ds(pl.multiple_of(step * tile, tile), tile)
        rows = recur_ref[at, :].astype(jnp.float32)
        longer = jnp.concatenate([tail, rows], axis=0)
        summed = jnp.zeros((tile, width), jnp.float32)
        for j in range(taps):
            start = 8 - (taps - 1) + j
            summed = summed + longer[start : start + tile] * taps_ref[j : j + 1, :]
        conv_out = summed.astype(jnp.bfloat16)
        rate_gate = jax.nn.sigmoid(
            jnp.dot(conv_out, decay_ref[...], preferred_element_type=jnp.float32)
        )
        input_gate = jax.nn.sigmoid(
            jnp.dot(conv_out, input_ref[...], preferred_element_type=jnp.float32)
        )
        log_a = rate_gate * rate_ref[...] + extra_ref[at, :]
        decay = jnp.exp(log_a)
        twice = 2.0 * log_a
        near_zero = -twice * (1.0 + twice * (0.5 + twice * (1.0 / 6.0)))
        left = jnp.where(twice > -0.03, near_zero, 1.0 - decay * decay)
        drive = jnp.sqrt(left) * input_gate * conv_out.astype(jnp.float32)
        steps = 1
        while steps < tile:
            drive = drive + decay * shifted(drive, steps, 0.0)
            decay = decay * shifted(decay, steps, 1.0)
            steps *= 2
        hidden = drive + decay * state
        branch = branch_ref[at, :].astype(jnp.float32)
        inner = 0.7978845608028654 * (branch + 0.044715 * branch * branch * branch)
        gelu = 0.5 * branch * (1.0 + jnp.tanh(inner))
        out_ref[at, :] = (gelu * hidden).astype(jnp.bfloat16)
        return rows[tile - 8 :], hidden[tile - 1 :]

    first = (jnp.zeros((8, width), jnp.float32), jnp.zeros((1, width), jnp.float32))
    lax.fori_loop(0, length // tile, body, first)


def block_diagonal(blocks, group):
    count, size, _ = blocks.shape
    parts = blocks.reshape(count // group, group, size, size)
    eye = jnp.eye(group, dtype=blocks.dtype)
    wide = parts[:, :, :, None, :] * eye[None, :, None, :, None]
    return wide.reshape(count // group, group * size, group * size)


def recurrence(recur, branch, taps, decay_blocks, input_blocks, decay_weight, extra):
    length, channels = recur.shape
    size = decay_blocks.shape[1]
    group = 1
    while (group * size) % 128 and decay_blocks.shape[0] % (2 * group) == 0:
        group *= 2
    width = group * size
    rate = (-RECURRENT_WIDTH * jax.nn.softplus(-decay_weight))[None]
    tile = ROW_TILE if length % ROW_TILE == 0 else length
    column = lambda i: (0, i)
    return pl.pallas_call(
        functools.partial(recurrence_kernel, tile=tile),
        grid=(channels // width,),
        in_specs=[
            pl.BlockSpec((length, width), column),
            pl.BlockSpec((length, width), column),
            pl.BlockSpec((taps.shape[0], width), column),
            pl.BlockSpec((None, width, width), lambda i: (i, 0, 0)),
            pl.BlockSpec((None, width, width), lambda i: (i, 0, 0)),
            pl.BlockSpec((1, width), column),
            pl.BlockSpec((length, 1), lambda i: (0, 0)),
        ],
        out_specs=pl.BlockSpec((length, width), column),
        out_shape=jax.ShapeDtypeStruct((length, channels), jnp.bfloat16),
        cost_estimate=pl.CostEstimate(
            flops=4 * length * channels * width * 4,
            bytes_accessed=6 * length * channels,
            transcendentals=6 * length * channels,
        ),
    )(
        recur,
        branch,
        taps,
        block_diagonal(decay_blocks, group),
        block_diagonal(input_blocks, group),
        rate,
        extra[:, None],
    )


def sublayer(residual, norm_scale_vector, first, second, out, middle):
    rows = gather_rows(jnp.stack(split_features(normed(residual, norm_scale_vector)), axis=1))
    own, other = rows[:, 0], rows[:, 1]

    def project(pair):
        return jnp.dot(own, pair[0], preferred_element_type=jnp.float32) + jnp.dot(
            other, pair[1], preferred_element_type=jnp.float32
        )

    hidden = middle(project(first), project(second))
    count = residual.shape[0]
    return join_features(
        project_scatter(hidden, out[0], count), project_scatter(hidden, out[1], count)
    )


def shards(
    tokens,
    first_block_norm_scale,
    first_block_gate_matrix,
    first_block_up_matrix,
    first_block_down_matrix,
    mixer_norm_scale,
    recurrent_input_matrix,
    output_gate_projection,
    convolution_kernel,
    decay_gate_blocks,
    input_gate_blocks,
    channel_decay_weight,
    position_decay_extra,
    mixer_output_matrix,
    second_block_norm_scale,
    second_block_gate_matrix,
    second_block_up_matrix,
    second_block_down_matrix,
):
    def feed_middle(gate_pre, up_pre):
        return (jax.nn.silu(gate_pre) * up_pre).astype(jnp.bfloat16)

    def mixer_middle(recur_pre, branch_pre):
        return recurrence(
            recur_pre.astype(jnp.bfloat16),
            branch_pre.astype(jnp.bfloat16),
            convolution_kernel,
            decay_gate_blocks,
            input_gate_blocks,
            channel_decay_weight,
            position_decay_extra,
        )

    first_weights = [
        gather_weight(first_block_gate_matrix, 0),
        gather_weight(first_block_up_matrix, 0),
        gather_weight(first_block_down_matrix, 1),
    ]
    mixer_weights = [
        gather_weight(recurrent_input_matrix, 0),
        gather_weight(output_gate_projection, 0),
        gather_weight(mixer_output_matrix, 1),
    ]
    second_weights = [
        gather_weight(second_block_gate_matrix, 0),
        gather_weight(second_block_up_matrix, 0),
        gather_weight(second_block_down_matrix, 1),
    ]
    residual = tokens
    change = sublayer(residual, first_block_norm_scale, *first_weights, feed_middle)
    residual = (residual.astype(jnp.float32) + 0.5 * change).astype(jnp.bfloat16)
    change = sublayer(residual, mixer_norm_scale, *mixer_weights, mixer_middle)
    residual = (residual.astype(jnp.float32) + change).astype(jnp.bfloat16)
    change = sublayer(residual, second_block_norm_scale, *second_weights, feed_middle)
    return (residual.astype(jnp.float32) + 0.5 * change).astype(jnp.bfloat16)


def solution(mesh):
    in_specs = (
        P(("fs", "tp"), None),
        P(),
        P("fs", "tp"),
        P("fs", "tp"),
        P("tp", "fs"),
        P(),
        P("fs", "tp"),
        P("fs", "tp"),
        P(None, "tp"),
        P("tp", None, None),
        P("tp", None, None),
        P("tp"),
        P("fs"),
        P("tp", "fs"),
        P(),
        P("fs", "tp"),
        P("fs", "tp"),
        P("tp", "fs"),
    )
    out_specs = P(("fs", "tp"), None)

    return jax.shard_map(shards, mesh=mesh, in_specs=in_specs, out_specs=out_specs, check_vma=False)
```
